32 devices in a mesh: dp: 4 (over y, x), kv: 4 (over z), tp: 2 (over core).
Axes of the slice: x: 2, y: 2, z: 4, core: 2. Of those that a mesh axis runs over, the one named last changes fastest.
Arguments:
- tokens: bfloat16 [32, 2048], P('dp', ('kv', 'tp')), may hold values from -30 to 30
- attention_gain: bfloat16 [2048], P(('kv', 'tp')), may hold values from 0.099609375 to 1.8984375
- query_one: bfloat16 [2048, 512], P('kv', 'tp'), may hold values from -0.125 to 0.125
- query_two: bfloat16 [2048, 512], P('kv', 'tp'), may hold values from -0.125 to 0.125
- key_one: bfloat16 [2048, 512], P('kv', 'tp'), may hold values from -2 to 2
- key_two: bfloat16 [2048, 512], P('kv', 'tp'), may hold values from -2 to 2
- value_weight: bfloat16 [2048, 1024], P('kv', 'tp'), may hold values from -0.125 to 0.125
- head_second_weight: float32 [8], P('tp'), may hold values from 0.3 to 0.8
- head_gain: float32 [128], replicated, may hold values from 0.1 to 1.9
- out_weight: bfloat16 [1024, 2048], P('tp', 'kv'), may hold values from -0.375 to 0.375
- mixer_gain: bfloat16 [2048], P(('kv', 'tp')), may hold values from 0.099609375 to 1.8984375
- gate_weight: bfloat16 [2048, 5632], P('kv', 'tp'), may hold values from -0.125 to 0.125
- up_weight: bfloat16 [2048, 5632], P('kv', 'tp'), may hold values from -0.125 to 0.125
- down_weight: bfloat16 [5632, 2048], P('tp', 'kv'), may hold values from -0.15625 to 0.15625
- key_cache: bfloat16 [32, 4096, 8, 128], P('dp', 'kv', 'tp'), may hold values from -240 to 240
- value_cache: bfloat16 [32, 4096, 8, 128], P('dp', 'kv', 'tp'), may hold values from -6 to 6
Outputs:
- layer_out: bfloat16 [32, 2048], P('dp', ('kv', 'tp'))
The draws below stay inside these ranges and needn't reach their ends.
All inputs are finite; a program needn't handle non-finite values.
Results may differ from the reference program's by a relative error of at most 0.02.
Values may be sent and summed in bfloat16 or wider, within the bound.
A program may use at most 64 MiB of HBM per device.

```python
import jax
import jax.numpy as jnp
from jax import lax

D = 2048
HEADS = 8
DH = 64
FF = 5632
POS_DEV = 1024
BATCH = 32
CACHE = 4096
N_TP = 2


def draw_tokens(key, part):
    columns = jnp.arange(D, dtype=jnp.float32)
    rising = jnp.exp(jnp.log(4.0) * columns / (D - 1))
    rough = jax.random.uniform(jax.random.fold_in(key, 11), (D,), jnp.float32, 0.5, 1.5)
    values = jnp.clip(jax.random.normal(jax.random.fold_in(key, 12), (BATCH, D), jnp.float32), -4.0, 4.0)
    return jnp.clip(values * rising * rough, -30.0, 30.0).astype(jnp.bfloat16)


def draw_key_cache(key, part):
    shape = (BATCH, CACHE, HEADS, 2 * DH)
    base = jnp.clip(jax.random.normal(jax.random.fold_in(key, 21), shape, jnp.float32) * 1.75, -10.5, 10.5)
    block_scale = jnp.exp(jax.random.uniform(jax.random.fold_in(key, 25), (BATCH, CACHE // POS_DEV, HEADS), jnp.float32, jnp.log(0.3), jnp.log(3.0)))
    base = base * jnp.repeat(block_scale, POS_DEV, axis=1)[..., None]
    row_boost = jnp.exp(jax.random.uniform(jax.random.fold_in(key, 24), (BATCH, 1, 1, 1), jnp.float32, jnp.log(30.0), jnp.log(60.0)))
    heavy_rows = (jnp.arange(BATCH) % 4 == 0)[:, None, None, None]
    base = jnp.where(heavy_rows, base * row_boost, base)
    return jnp.clip(base, -240.0, 240.0).astype(jnp.bfloat16)


def shard_levels(rng, shape, cuts, least, largest):
    def one(dim, parts):
        heights = jax.random.uniform(jax.random.fold_in(jax.random.fold_in(rng, 6), dim), (parts,), jnp.float32, least / len(cuts), largest / len(cuts))
        return jnp.repeat(jnp.exp(heights), shape[dim] // parts).reshape((-1,) + (1,) * (len(shape) - dim - 1))

    loudness = one(*cuts[0])
    for cut in cuts[1:]:
        loudness = loudness * one(*cut)
    return loudness


def gaussian(stream_key, shape, spread, most, shards=(), kind=jnp.bfloat16):
    values = spread * jax.random.normal(stream_key, shape, jnp.float32)
    if shards:
        values = values * shard_levels(stream_key, shape, shards, -0.22, 0.18)
    return jnp.clip(values, -most, most).astype(kind)


def setup_inputs(seed: int = 0) -> dict:
    seeds = jax.random.split(jax.random.key(seed), 17)
    return {
        "tokens": draw_tokens(jax.random.fold_in(seeds[16], 71), 0),
        "attention_gain": jnp.clip(1.0 + 0.18 * jax.random.normal(seeds[1], (D,), jnp.float32), 0.099609375, 1.8984375).astype(jnp.bfloat16),
        "query_one": gaussian(seeds[2], (D, HEADS * DH), D ** -0.5, 0.125, ((0, 4), (1, 2))),
        "query_two": gaussian(seeds[3], (D, HEADS * DH), D ** -0.5, 0.125, ((0, 4), (1, 2))),
        "key_one": gaussian(seeds[4], (D, HEADS * DH), (D // 256) ** -0.5, 2.0, ((0, 4), (1, 2))),
        "key_two": gaussian(seeds[5], (D, HEADS * DH), (D // 256) ** -0.5, 2.0, ((0, 4), (1, 2))),
        "value_weight": gaussian(seeds[6], (D, HEADS * 2 * DH), D ** -0.5, 0.125, ((0, 4), (1, 2))),
        "head_second_weight": jnp.clip(0.3 + 0.5 * jax.random.uniform(seeds[7], (HEADS,), jnp.float32) ** shard_levels(seeds[7], (HEADS,), ((0, 2),), -0.2, 0.2), 0.3, 0.8),
        "head_gain": jnp.clip(1.0 + 0.18 * jax.random.normal(seeds[8], (2 * DH,), jnp.float32), 0.1, 1.9),
        "out_weight": gaussian(seeds[9], (HEADS * 2 * DH, D), (HEADS * DH // 2) ** -0.5, 0.375, ((0, 2), (1, 4))),
        "mixer_gain": jnp.clip(1.0 + 0.18 * jax.random.normal(seeds[10], (D,), jnp.float32), 0.099609375, 1.8984375).astype(jnp.bfloat16),
        "gate_weight": gaussian(seeds[11], (D, FF), D ** -0.5, 0.125, ((0, 4), (1, 2))),
        "up_weight": gaussian(seeds[12], (D, FF), D ** -0.5, 0.125, ((0, 4), (1, 2))),
        "down_weight": gaussian(seeds[13], (FF, D), (FF // 4) ** -0.5, 0.15625, ((0, 2), (1, 4))),
        "key_cache": draw_key_cache(jax.random.fold_in(seeds[16], 71), 0),
        "value_cache": gaussian(seeds[15], (BATCH, CACHE, HEADS, 2 * DH), 1.0, 6.0, ((0, 4), (1, 4), (2, 2))),
    }


NORM_EPSILON = 1e-06
HEAD_EPSILON = 1e-05
HEAD_SCALE = 0.8
ROTARY_BASE = 10000.0

def rotate(vectors, position):
    half_width = vectors.shape[-1] // 2
    frequency = 1.0 / ROTARY_BASE ** (jnp.arange(half_width, dtype=jnp.float32) / half_width)
    angles = position * frequency
    cosine = jnp.cos(angles)
    sine_value = jnp.sin(angles)
    lead_half = vectors[..., :half_width]
    tail_half = vectors[..., half_width:]
    return jnp.concatenate([lead_half * cosine - tail_half * sine_value, tail_half * cosine + lead_half * sine_value], axis=-1)

def rounded(values):
    return lax.optimization_barrier(values.astype(jnp.bfloat16)).astype(jnp.float32)

def grouped_product(left, right, groups):
    group_width = left.shape[1] // groups
    result = jnp.zeros((left.shape[0], right.shape[1]), jnp.float32)
    for group_index in range(groups):
        group_term = jnp.dot(left[:, group_index * group_width:(group_index + 1) * group_width], right[group_index * group_width:(group_index + 1) * group_width], preferred_element_type=jnp.float32)
        result = result + rounded(group_term)
    return result

def reference(tokens, attention_gain, query_one, query_two, key_one, key_two, value_weight, head_second_weight, head_gain, out_weight, mixer_gain, gate_weight, up_weight, down_weight, key_cache, value_cache):
    position = jnp.float32(CACHE)
    score_scale = DH ** (-0.5)
    token_values = tokens.astype(jnp.float32)
    row_ratio = lax.rsqrt(lax.optimization_barrier(jnp.mean(token_values * token_values, axis=1, keepdims=True)) + NORM_EPSILON)
    scaled = (token_values * attention_gain.astype(jnp.float32)).astype(jnp.bfloat16)

    def project(weight_matrix):
        return jnp.dot(scaled, weight_matrix, preferred_element_type=jnp.float32) * row_ratio

    def paired(lead_matrix, tail_matrix):
        both = jnp.stack([project(lead_matrix).reshape(BATCH, HEADS, DH), project(tail_matrix).reshape(BATCH, HEADS, DH)], axis=2)
        return rotate(both, position).astype(jnp.bfloat16)
    queries = paired(query_one, query_two)
    new_keys = paired(key_one, key_two)
    new_values = project(value_weight).astype(jnp.bfloat16).reshape(BATCH, HEADS, 2 * DH)

    def one_sequence(operands):
        query, new_key, new_value, cached_keys, cached_values = operands
        query_entries = query.astype(jnp.float32)
        key_entries = cached_keys.astype(jnp.float32).reshape(CACHE, HEADS, 2, DH)
        logit_scores = jnp.einsum('tvs,ntvs->tvn', query_entries, key_entries) * score_scale
        own_score = lax.optimization_barrier(jnp.sum(query_entries * new_key.astype(jnp.float32), axis=-1)) * score_scale
        peak_score = jnp.maximum(lax.optimization_barrier(jnp.max(logit_scores, axis=-1)), own_score)
        exponent = jnp.exp(logit_scores - peak_score[..., None])
        own_weight = jnp.exp(own_score - peak_score)
        weight_sum = lax.optimization_barrier(jnp.sum(exponent, axis=-1)) + own_weight
        weighted = jnp.einsum('hmp,phe->hme', rounded(exponent), cached_values.astype(jnp.float32))
        weighted = weighted + own_weight[..., None] * new_value.astype(jnp.float32)[:, None, :]
        averaged = weighted / weight_sum[..., None]
        difference = averaged[:, 0] - head_second_weight[:, None] * averaged[:, 1]
        inverse_norm = lax.rsqrt(lax.optimization_barrier(jnp.mean(difference * difference, axis=-1, keepdims=True)) + HEAD_EPSILON)
        return (difference * inverse_norm * head_gain[None, :] * HEAD_SCALE).astype(jnp.bfloat16)
    attended = lax.map(one_sequence, (queries, new_keys, new_values, key_cache, value_cache))
    attended = attended.reshape(BATCH, HEADS * 2 * DH)
    attention_out = grouped_product(attended, out_weight, N_TP)
    mixed = (token_values + attention_out).astype(jnp.bfloat16)
    mixed_values = mixed.astype(jnp.float32)
    mixer_ratio = lax.rsqrt(lax.optimization_barrier(jnp.mean(mixed_values * mixed_values, axis=1, keepdims=True)) + NORM_EPSILON)
    mixer_scaled = (mixed_values * mixer_gain.astype(jnp.float32)).astype(jnp.bfloat16)
    gate_values = jnp.dot(mixer_scaled, gate_weight, preferred_element_type=jnp.float32) * mixer_ratio
    up_values = jnp.dot(mixer_scaled, up_weight, preferred_element_type=jnp.float32) * mixer_ratio
    hidden_state = (jax.nn.silu(gate_values) * up_values).astype(jnp.bfloat16)
    mixer_out = grouped_product(hidden_state, down_weight, N_TP)
    return (mixed_values + mixer_out).astype(jnp.bfloat16)
```

```python
import functools

import jax
import jax.numpy as jnp
import numpy as np
from jax import lax
from jax.experimental import pallas as pl
from jax.experimental.pallas import tpu as pltpu
from jax.sharding import PartitionSpec as P

DH = 64
LANES = 128

NORM_EPSILON = 1e-06
HEAD_EPSILON = 1e-05
HEAD_SCALE = 0.8
ROTARY_BASE = 10000.0

F32 = jnp.float32
BF16 = jnp.bfloat16


def rotary_table(position, local_heads):
    half = DH // 2
    frequency = np.float32(1.0) / np.float32(ROTARY_BASE) ** (np.arange(half, dtype=np.float32) / np.float32(half))
    angles = (np.float32(position) * frequency).astype(np.float32).astype(np.float64)
    cosine = np.concatenate([np.cos(angles), np.cos(angles)])
    sine = np.concatenate([-np.sin(angles), np.sin(angles)])
    return np.stack([np.tile(cosine, local_heads), np.tile(sine, local_heads)]).astype(np.float32)


def dot(left, right):
    return jnp.dot(left, right, preferred_element_type=F32)


def layer(
    n, pack, table, second_weight, head_gain, q1_h, q2_h, k1_h, k2_h, v_h, out_h, gate_h, up_h,
    down_h, key_h, value_h, result,
    tok, q1_w, q2_w, k1_w, k2_w, v_w, out_w, gate_w, up_w, down_w, keys, values,
    q_part, kv_part, q_pad, scores, acc, stats, total, peak_s, sum_s, att_x, sq, gu_out, gu_in,
    hid, mix_x, load, key_sem, value_sem, tp_send, tp_recv, kv_send, kv_recv,
):
    rows = pack.shape[0] - 8
    local_heads = q1_h.shape[1] // DH
    maps = 2 * local_heads
    me = lax.axis_index("kv")
    side = lax.axis_index("tp")
    other = 1 - side
    width = pack.shape[1]
    model_width = width * 2 * n
    hidden_width = gate_h.shape[1]
    chunk = hid.shape[2]

    def fetch(source, target, sem):
        copy = pltpu.make_async_copy(source, target, sem)
        copy.start()
        return copy

    pack_copy = fetch(pack, tok.at[side], load.at[0])
    loads = [
        fetch(source, target, load.at[1 + i])
        for i, (source, target) in enumerate(
            ((q1_h, q1_w), (q2_h, q2_w), (k1_h, k1_w), (k2_h, k2_w), (v_h, v_w))
        )
    ]
    key_copies = [fetch(key_h.at[b], keys.at[b], key_sem.at[b]) for b in range(rows)]
    value_copies = [fetch(value_h.at[b], values.at[b], value_sem.at[b]) for b in range(rows)]
    out_copy = fetch(out_h, out_w, load.at[6])
    gate_copy = fetch(gate_h, gate_w.at[:, pl.ds(0, hidden_width)], load.at[7])
    up_copy = fetch(up_h, up_w.at[:, pl.ds(0, hidden_width)], load.at[8])
    down_copy = fetch(down_h, down_w, load.at[9])

    barrier = pltpu.get_barrier_semaphore()
    pl.semaphore_signal(barrier, inc=1, device_id={"tp": other})
    for d in range(1, n):
        pl.semaphore_signal(barrier, inc=1, device_id={"kv": lax.rem(me + d, n)})
    pl.semaphore_wait(barrier, n)

    def swap(phase, source, target):
        copy = pltpu.make_async_remote_copy(
            src_ref=source, dst_ref=target, send_sem=tp_send.at[phase],
            recv_sem=tp_recv.at[phase], device_id={"tp": other},
        )
        copy.start()
        return copy

    def push(phase, d, source, target):
        copy = pltpu.make_async_remote_copy(
            src_ref=source, dst_ref=target, send_sem=kv_send.at[phase, d - 1],
            recv_sem=kv_recv.at[phase, d - 1], device_id={"kv": lax.rem(me + d, n)},
        )
        copy.start()
        return copy

    def share(phase, buffer):
        return [push(phase, d, buffer.at[me], buffer.at[me]) for d in range(1, n)]

    def landed(copies):
        for copy in copies:
            copy.wait_recv()

    sent = []
    tok_swap = swap(0, pack, tok.at[side])
    if chunk * n > hidden_width:
        pad = chunk * n - hidden_width
        gate_w[:, hidden_width:] = jnp.zeros((gate_w.shape[0], pad), BF16)
        up_w[:, hidden_width:] = jnp.zeros((up_w.shape[0], pad), BF16)
    pack_copy.wait()
    tok_swap.wait_recv()
    block = jnp.concatenate([tok[0], tok[1]], axis=1)
    token_values = block[:rows]
    scaled = (token_values * block[rows : rows + 1]).astype(BF16)
    mixer_gain = block[rows + 1 : rows + 2]

    def lane_total(x):
        return jnp.broadcast_to(jnp.sum(x * x, axis=1, keepdims=True), (rows, LANES))

    qw = q1_h.shape[1]
    vw = v_h.shape[1]
    loads[0].wait()
    q_part[me, :, :qw] = dot(scaled, q1_w[...])
    loads[1].wait()
    q_part[me, :, qw : 2 * qw] = dot(scaled, q2_w[...])
    q_part[me, :, 2 * qw :] = lane_total(token_values)
    q_shared = share(0, q_part)
    loads[2].wait()
    kv_part[me, :, :qw] = dot(scaled, k1_w[...])
    loads[3].wait()
    kv_part[me, :, qw : 2 * qw] = dot(scaled, k2_w[...])
    loads[4].wait()
    kv_part[me, :, 2 * qw :] = dot(scaled, v_w[...])
    kv_shared = share(1, kv_part)

    cosine = table[0:1, :]
    sine = table[1:2, :]
    lane = lax.broadcasted_iota(jnp.int32, (rows, qw), 1)
    lead = lax.rem(lane, DH) < DH // 2
    tile_lane = lax.broadcasted_iota(jnp.int32, (rows, LANES), 1)
    low = tile_lane < DH

    def rotated(x):
        turned = jnp.where(lead, pltpu.roll(x, qw - DH // 2, 1), pltpu.roll(x, DH // 2, 1))
        return (x * cosine + turned * sine).astype(BF16).astype(F32)

    def padded(first, second):
        tiles = []
        for h in range(local_heads):
            at = (h // 2) * LANES
            one = first[:, at : at + LANES]
            two = second[:, at : at + LANES]
            if h % 2:
                one = pltpu.roll(one, DH, 1)
            else:
                two = pltpu.roll(two, DH, 1)
            tiles.append(jnp.where(low, one, 0.0))
            tiles.append(jnp.where(low, 0.0, two))
        return tiles

    landed(q_shared)
    q_sum = functools.reduce(jnp.add, [q_part[s] for s in range(n)])
    ratio = lax.rsqrt(q_sum[:, 2 * qw : 2 * qw + 1] / model_width + NORM_EPSILON)
    queries = padded(rotated(q_sum[:, :qw] * ratio), rotated(q_sum[:, qw : 2 * qw] * ratio))
    for i in range(maps):
        q_pad[:, i, :] = queries[i]

    span = keys.shape[1]
    score_scale = DH ** (-0.5)
    row_head = lax.broadcasted_iota(jnp.int32, (maps, span), 0) // 2
    col_head = lax.rem(lax.broadcasted_iota(jnp.int32, (maps, span), 1), local_heads)
    mine = row_head == col_head
    stat_lane = lax.broadcasted_iota(jnp.int32, (maps, LANES), 1)
    stat = jnp.zeros((maps, LANES), F32)
    for b in range(rows):
        key_copies[b].wait()
        raw = lax.dot_general(
            q_pad[b].astype(BF16), keys[b], (((1,), (1,)), ((), ())), preferred_element_type=F32
        )
        scores[b] = jnp.where(mine, raw * score_scale, -jnp.inf)
    for b in range(rows):
        value_copies[b].wait()
        logit = scores[b]
        peak = jnp.max(logit, axis=1, keepdims=True)
        weight = jnp.exp(logit - peak)
        weight_sum = jnp.sum(weight, axis=1, keepdims=True)
        acc[me, b] = dot(weight.astype(BF16), values[b])
        stat = jnp.where(stat_lane == b, peak, stat)
        stat = jnp.where(stat_lane == rows + b, weight_sum, stat)
    stats[me] = stat
    acc_shared = share(2, acc)
    stat_shared = share(3, stats)

    landed(kv_shared)
    kv_sum = functools.reduce(jnp.add, [kv_part[s] for s in range(n)])
    new_keys = padded(rotated(kv_sum[:, :qw] * ratio), rotated(kv_sum[:, qw : 2 * qw] * ratio))
    new_values = (kv_sum[:, 2 * qw :] * ratio).astype(BF16).astype(F32)
    own = [
        jnp.sum(queries[i] * new_keys[i], axis=1, keepdims=True) * score_scale for i in range(maps)
    ]

    landed(stat_shared)
    every = [stats[s] for s in range(n)]
    top = functools.reduce(jnp.maximum, every)
    is_peak = stat_lane < rows
    factor = [jnp.exp(jnp.where(is_peak, every[s] - top, 0.0)) for s in range(n)]
    sums = [pltpu.roll(every[s], LANES - rows, 1) for s in range(n)]
    mass = functools.reduce(jnp.add, [factor[s] * sums[s] for s in range(n)])
    for b in range(rows):
        peak_s[b] = jnp.broadcast_to(top[:, b : b + 1], (maps, LANES))
        sum_s[b] = jnp.broadcast_to(mass[:, b : b + 1], (maps, LANES))
    landed(acc_shared)
    for b in range(rows):
        total[b] = functools.reduce(
            jnp.add, [acc[s, b] * factor[s][:, b : b + 1] for s in range(n)]
        )

    averaged = []
    for i in range(maps):
        peak = peak_s[:, i, :]
        final = jnp.maximum(peak, own[i])
        keep = jnp.exp(peak - final)
        own_weight = jnp.exp(own[i] - final)
        at = (i // 2) * 2 * DH
        over = total[:, i, :] * keep + own_weight * new_values[:, at : at + 2 * DH]
        averaged.append(over / (sum_s[:, i, :] * keep + own_weight))
    heads = []
    gain = head_gain[...]
    for h in range(local_heads):
        difference = averaged[2 * h] - second_weight[0, h] * averaged[2 * h + 1]
        inverse = lax.rsqrt(jnp.mean(difference * difference, axis=1, keepdims=True) + HEAD_EPSILON)
        heads.append((difference * inverse * gain * HEAD_SCALE).astype(BF16))
    attended = jnp.concatenate(heads, axis=1)

    out_copy.wait()
    att_x[side] = dot(attended, out_w[...]).astype(BF16)
    att_swap = swap(1, att_x.at[side], att_x.at[side])
    att_swap.wait_recv()
    mixed = (token_values + (att_x[0].astype(F32) + att_x[1].astype(F32))).astype(BF16)
    mixed_values = mixed.astype(F32)
    sq[me] = lane_total(mixed_values)
    sq_shared = share(4, sq)
    mixer_scaled = (mixed_values * mixer_gain).astype(BF16)

    gate_copy.wait()
    up_copy.wait()
    gu_shared = []
    for d in range(1, n + 1):
        target = lax.rem(me + d, n)
        columns = pl.ds(pl.multiple_of(target * chunk, LANES), chunk)
        gate_part = dot(mixer_scaled, gate_w[:, columns])
        up_part = dot(mixer_scaled, up_w[:, columns])
        if d < n:
            gu_out[d - 1, :, :chunk] = gate_part.astype(BF16)
            gu_out[d - 1, :, chunk:] = up_part.astype(BF16)
            gu_shared.append(push(5, d, gu_out.at[d - 1], gu_in.at[d - 1]))
    landed(sq_shared)
    mixer_total = functools.reduce(jnp.add, [sq[s] for s in range(n)])[:, :1]
    mixer_ratio = lax.rsqrt(mixer_total / model_width + NORM_EPSILON)
    for d in range(1, n):
        gu_shared[d - 1].wait_recv()
        gate_part = gate_part + gu_in[d - 1, :, :chunk].astype(F32)
        up_part = up_part + gu_in[d - 1, :, chunk:].astype(F32)
    gate = gate_part * mixer_ratio
    hid[me] = (gate / (1.0 + jnp.exp(-gate)) * (up_part * mixer_ratio)).astype(BF16)
    hid_shared = share(6, hid)
    down_copy.wait()
    landed(hid_shared)
    term = None
    for s in range(n):
        depth = min(chunk, hidden_width - s * chunk)
        if depth > 0:
            piece = dot(hid[s][:, :depth], down_w[pl.ds(s * chunk, depth), :])
            term = piece if term is None else term + piece
    mix_x[side] = term.astype(BF16)
    mix_swap = swap(2, mix_x.at[side], mix_x.at[side])
    mix_swap.wait_recv()
    full = mixed_values + (mix_x[0].astype(F32) + mix_x[1].astype(F32))
    result[...] = jnp.where(side == 0, full[:, :width], full[:, width:]).astype(BF16)

    for copy in (
        [tok_swap, att_swap, mix_swap]
        + q_shared + kv_shared + acc_shared + stat_shared + sq_shared + gu_shared + hid_shared
    ):
        copy.wait_send()


def shards(
    n, tokens, attention_gain, query_one, query_two, key_one, key_two, value_weight,
    head_second_weight, head_gain, out_weight, mixer_gain, gate_weight, up_weight, down_weight,
    key_cache, value_cache,
):
    rows, width = tokens.shape
    positions, local_heads = key_cache.shape[1:3]
    maps = 2 * local_heads
    qw = query_one.shape[1]
    block = 2 * width
    hidden = gate_weight.shape[1]
    chunk = -(-hidden // (LANES * n)) * LANES
    pack = jnp.concatenate(
        [
            tokens.astype(F32),
            attention_gain.astype(F32)[None],
            mixer_gain.astype(F32)[None],
            jnp.zeros((6, width), F32),
        ],
        axis=0,
    )
    table = jnp.asarray(rotary_table(positions * n, local_heads))
    span = positions * local_heads
    key_rows = key_cache.reshape(rows, span, 2 * DH)
    value_rows = value_cache.reshape(rows, span, 2 * DH)
    anywhere = pl.BlockSpec(memory_space=pl.ANY)
    inside = pl.BlockSpec(memory_space=pltpu.VMEM)
    vmem = pltpu.VMEM
    dma = pltpu.SemaphoreType.DMA
    weights = [query_one, query_two, key_one, key_two, value_weight, out_weight]
    return pl.pallas_call(
        functools.partial(layer, n),
        out_shape=jax.ShapeDtypeStruct((rows, width), BF16),
        in_specs=[anywhere, inside, pl.BlockSpec(memory_space=pltpu.SMEM), inside] + [anywhere] * 11,
        out_specs=inside,
        scratch_shapes=[vmem((2, rows + 8, width), F32)]
        + [vmem(w.shape, BF16) for w in weights]
        + [
            vmem((block, chunk * n), BF16),
            vmem((block, chunk * n), BF16),
            vmem(down_weight.shape, BF16),
            vmem(key_rows.shape, BF16),
            vmem(value_rows.shape, BF16),
            vmem((n, rows, 2 * qw + LANES), F32),
            vmem((n, rows, 2 * qw + value_weight.shape[1]), F32),
            vmem((rows, maps, LANES), F32),
            vmem((rows, maps, span), F32),
            vmem((n, rows, maps, LANES), F32),
            vmem((n, maps, LANES), F32),
            vmem((rows, maps, LANES), F32),
            vmem((rows, maps, LANES), F32),
            vmem((rows, maps, LANES), F32),
            vmem((2, rows, block), BF16),
            vmem((n, rows, LANES), F32),
            vmem((n - 1, rows, 2 * chunk), BF16),
            vmem((n - 1, rows, 2 * chunk), BF16),
            vmem((n, rows, chunk), BF16),
            vmem((2, rows, block), BF16),
            dma((10,)),
            dma((rows,)),
            dma((rows,)),
            dma((3,)),
            dma((3,)),
            dma((7, n - 1)),
            dma((7, n - 1)),
        ],
        compiler_params=pltpu.CompilerParams(
            collective_id=0, has_side_effects=True, vmem_limit_bytes=60 * 1024 * 1024
        ),
    )(
        pack, table, head_second_weight[None], head_gain[None], query_one, query_two, key_one,
        key_two, value_weight, out_weight, gate_weight, up_weight, down_weight, key_rows, value_rows,
    )


def solution(mesh):
    placed = (
        P("dp", ("kv", "tp")),
        P(("kv", "tp")),
        P("kv", "tp"),
        P("kv", "tp"),
        P("kv", "tp"),
        P("kv", "tp"),
        P("kv", "tp"),
        P("tp"),
        P(),
        P("tp", "kv"),
        P(("kv", "tp")),
        P("kv", "tp"),
        P("kv", "tp"),
        P("tp", "kv"),
        P("dp", "kv", "tp", None),
        P("dp", "kv", "tp", None),
    )
    return jax.shard_map(
        functools.partial(shards, mesh.shape["kv"]),
        mesh=mesh, in_specs=placed, out_specs=P("dp", ("kv", "tp")), check_vma=False,
    )
```

```python
import functools

import jax
import jax.numpy as jnp
import numpy as np
from jax import lax
from jax.experimental import pallas as pl
from jax.experimental.pallas import tpu as pltpu
from jax.sharding import PartitionSpec as P

DH = 64
LANES = 128

NORM_EPSILON = 1e-06
HEAD_EPSILON = 1e-05
HEAD_SCALE = 0.8
ROTARY_BASE = 10000.0

F32 = jnp.float32
BF16 = jnp.bfloat16


def rotary_table(position, local_heads):
    half = DH // 2
    frequency = np.float32(1.0) / np.float32(ROTARY_BASE) ** (np.arange(half, dtype=np.float32) / np.float32(half))
    angles = (np.float32(position) * frequency).astype(np.float32).astype(np.float64)
    cosine = np.concatenate([np.cos(angles), np.cos(angles)])
    sine = np.concatenate([-np.sin(angles), np.sin(angles)])
    return np.stack([np.tile(cosine, local_heads), np.tile(sine, local_heads)]).astype(np.float32)


def peer_order(me, n):
    assert n & (n - 1) == 0
    order = []
    for flip in range(n - 1, 0, -1):
        target = me
        bit = 1
        while bit < n:
            if flip & bit:
                target = target + bit - 2 * bit * lax.rem(me // bit, 2)
            bit *= 2
        order.append(target)
    return order


def dot(left, right):
    return jnp.dot(left, right, preferred_element_type=F32)


def layer(
    n, tokens_h, first_gain_h, second_gain_h, table_h, second_weight_h, head_gain_h, q1_h, q2_h, k1_h, k2_h, v_h, out_h, gate_h, up_h,
    down_h, key_h, value_h, result,
    raw_tokens, raw_first, raw_second, table, second_weight, head_gain, tok, q1_w, q2_w, k1_w, k2_w, v_w, out_w, gate_w, up_w, down_w, keys, values,
    q_part, kv_part, q_pad, scores, acc, stats, total, peak_s, sum_s, att_x, sq, gu_out, gu_in,
    hid, mix_x, load, key_sem, value_sem, tp_send, tp_recv, kv_send, kv_recv,
):
    rows, width = tokens_h.shape
    local_heads = q1_h.shape[1] // DH
    maps = 2 * local_heads
    me = lax.axis_index("kv")
    side = lax.axis_index("tp")
    other = 1 - side
    model_width = width * 2 * n
    hidden_width = gate_h.shape[1]
    chunk = hid.shape[2]

    peers = peer_order(me, n)
    barrier = pltpu.get_barrier_semaphore()
    for target in peers:
        pl.semaphore_signal(barrier, inc=1, device_id={"kv": target})
    pl.semaphore_signal(barrier, inc=1, device_id={"tp": other})

    def fetch(source, target, sem):
        copy = pltpu.make_async_copy(source, target, sem)
        copy.start()
        return copy

    small = [
        fetch(source, target, load.at[10 + i])
        for i, (source, target) in enumerate(
            (
                (tokens_h, raw_tokens), (first_gain_h, raw_first), (second_gain_h, raw_second),
                (table_h, table), (second_weight_h, second_weight), (head_gain_h, head_gain),
            )
        )
    ]
    loads = [
        fetch(source, target, load.at[i])
        for i, (source, target) in enumerate(
            ((q1_h, q1_w), (q2_h, q2_w), (k1_h, k1_w), (k2_h, k2_w), (v_h, v_w))
        )
    ]
    for copy in small:
        copy.wait()
    tok[side, :rows] = raw_tokens[...].astype(F32)
    tok[side, rows : rows + 1] = raw_first[...].astype(F32).reshape(1, width)
    tok[side, rows + 1 : rows + 2] = raw_second[...].astype(F32).reshape(1, width)
    tok[side, rows + 2 :] = jnp.zeros((6, width), F32)
    pl.semaphore_wait(barrier, n)

    def swap(phase, source, target):
        copy = pltpu.make_async_remote_copy(
            src_ref=source, dst_ref=target, send_sem=tp_send.at[phase],
            recv_sem=tp_recv.at[phase], device_id={"tp": other},
        )
        copy.start()
        return copy

    def push(phase, k, source, target):
        copy = pltpu.make_async_remote_copy(
            src_ref=source, dst_ref=target, send_sem=kv_send.at[phase, k],
            recv_sem=kv_recv.at[phase, k], device_id={"kv": peers[k]},
        )
        copy.start()
        return copy

    def share(phase, buffer):
        return [push(phase, k, buffer.at[me], buffer.at[me]) for k in range(n - 1)]

    def landed(copies):
        for copy in copies:
            copy.wait_recv()

    sent = []
    tok_swap = swap(0, tok.at[side], tok.at[side])
    key_copies = [
        fetch(key_h.at[b], keys.at[b // 2, :, pl.ds(b % 2 * LANES, LANES)], key_sem.at[b])
        for b in range(rows)
    ]
    value_copies = [
        fetch(value_h.at[b], values.at[b // 2, :, pl.ds(b % 2 * LANES, LANES)], value_sem.at[b])
        for b in range(rows)
    ]
    out_copy = fetch(out_h, out_w, load.at[6])
    gate_copy = fetch(gate_h, gate_w.at[:, pl.ds(0, hidden_width)], load.at[7])
    up_copy = fetch(up_h, up_w.at[:, pl.ds(0, hidden_width)], load.at[8])
    down_copy = fetch(down_h, down_w, load.at[9])
    if chunk * n > hidden_width:
        pad = chunk * n - hidden_width
        gate_w[:, hidden_width:] = jnp.zeros((gate_w.shape[0], pad), BF16)
        up_w[:, hidden_width:] = jnp.zeros((up_w.shape[0], pad), BF16)
    tok_swap.wait_recv()
    block = jnp.concatenate([tok[0], tok[1]], axis=1)
    token_values = block[:rows]
    scaled = (token_values * block[rows : rows + 1]).astype(BF16)
    mixer_gain = block[rows + 1 : rows + 2]

    def lane_total(x):
        return jnp.broadcast_to(jnp.sum(x * x, axis=1, keepdims=True), (rows, LANES))

    qw = q1_h.shape[1]
    vw = v_h.shape[1]
    loads[0].wait()
    q_part[me, :, :qw] = dot(scaled, q1_w[...])
    loads[1].wait()
    q_part[me, :, qw : 2 * qw] = dot(scaled, q2_w[...])
    q_part[me, :, 2 * qw :] = lane_total(token_values)
    q_shared = share(0, q_part)
    loads[2].wait()
    kv_part[me, :, :qw] = dot(scaled, k1_w[...])
    loads[3].wait()
    kv_part[me, :, qw : 2 * qw] = dot(scaled, k2_w[...])
    loads[4].wait()
    kv_part[me, :, 2 * qw :] = dot(scaled, v_w[...])
    kv_shared = share(1, kv_part)

    cosine = table[0:1, :]
    sine = table[1:2, :]
    lane = lax.broadcasted_iota(jnp.int32, (rows, qw), 1)
    lead = lax.rem(lane, DH) < DH // 2
    tile_lane = lax.broadcasted_iota(jnp.int32, (rows, LANES), 1)
    low = tile_lane < DH

    def rotated(x):
        turned = jnp.where(lead, pltpu.roll(x, qw - DH // 2, 1), pltpu.roll(x, DH // 2, 1))
        return (x * cosine + turned * sine).astype(BF16).astype(F32)

    def padded(first, second):
        tiles = []
        for h in range(local_heads):
            at = (h // 2) * LANES
            one = first[:, at : at + LANES]
            two = second[:, at : at + LANES]
            if h % 2:
                one = pltpu.roll(one, DH, 1)
            else:
                two = pltpu.roll(two, DH, 1)
            tiles.append(jnp.where(low, one, 0.0))
            tiles.append(jnp.where(low, 0.0, two))
        return tiles

    landed(q_shared)
    q_sum = functools.reduce(jnp.add, [q_part[s] for s in range(n)])
    ratio = lax.rsqrt(q_sum[:, 2 * qw : 2 * qw + 1] / model_width + NORM_EPSILON)
    queries = padded(rotated(q_sum[:, :qw] * ratio), rotated(q_sum[:, qw : 2 * qw] * ratio))
    for i in range(maps):
        q_pad[:, i, :] = queries[i]

    span = keys.shape[1]
    score_scale = DH ** (-0.5)
    pair = 2 * maps
    row_head = lax.rem(lax.broadcasted_iota(jnp.int32, (pair, span), 0), maps) // 2
    col_head = lax.rem(lax.broadcasted_iota(jnp.int32, (pair, span), 1), local_heads)
    mine = row_head == col_head
    stat_lane = lax.broadcasted_iota(jnp.int32, (maps, LANES), 1)
    stat = jnp.zeros((maps, LANES), F32)
    blank = jnp.zeros((maps, LANES), F32)
    acc_shared = []

    def score(g):
        key_copies[2 * g].wait()
        key_copies[2 * g + 1].wait()
        query = jnp.concatenate(
            [
                jnp.concatenate([q_pad[2 * g], blank], axis=1),
                jnp.concatenate([blank, q_pad[2 * g + 1]], axis=1),
            ],
            axis=0,
        ).astype(BF16)
        raw = lax.dot_general(
            query, keys[g], (((1,), (1,)), ((), ())), preferred_element_type=F32
        )
        scores[g] = jnp.where(mine, raw * score_scale, -jnp.inf)

    groups = rows // 2
    score(0)
    for g in range(groups):
        if g + 1 < groups:
            score(g + 1)
        value_copies[2 * g].wait()
        value_copies[2 * g + 1].wait()
        logit = scores[g]
        peak = jnp.max(logit, axis=1, keepdims=True)
        weight = jnp.exp(logit - peak)
        weight_sum = jnp.sum(weight, axis=1, keepdims=True)
        both = dot(weight.astype(BF16), values[g])
        for j in range(2):
            part = slice(j * maps, (j + 1) * maps)
            acc[me, 2 * g + j] = both[part, j * LANES : (j + 1) * LANES]
            stat = jnp.where(stat_lane == 2 * g + j, peak[part], stat)
            stat = jnp.where(stat_lane == rows + 2 * g + j, weight_sum[part], stat)
        if g + 1 == groups:
            stats[me] = stat
            stat_shared = share(3, stats)
        pieces = acc.at[me, pl.ds(2 * g, 2)]
        acc_shared += [push(7 + g, k, pieces, pieces) for k in range(n - 1)]

    landed(kv_shared)
    kv_sum = functools.reduce(jnp.add, [kv_part[s] for s in range(n)])
    new_keys = padded(rotated(kv_sum[:, :qw] * ratio), rotated(kv_sum[:, qw : 2 * qw] * ratio))
    new_values = (kv_sum[:, 2 * qw :] * ratio).astype(BF16).astype(F32)
    own = [
        jnp.sum(queries[i] * new_keys[i], axis=1, keepdims=True) * score_scale for i in range(maps)
    ]

    landed(stat_shared)
    every = [stats[s] for s in range(n)]
    top = functools.reduce(jnp.maximum, every)
    is_peak = stat_lane < rows
    factor = [jnp.exp(jnp.where(is_peak, every[s] - top, 0.0)) for s in range(n)]
    sums = [pltpu.roll(every[s], LANES - rows, 1) for s in range(n)]
    mass = functools.reduce(jnp.add, [factor[s] * sums[s] for s in range(n)])
    for b in range(rows):
        peak_s[b] = jnp.broadcast_to(top[:, b : b + 1], (maps, LANES))
        sum_s[b] = jnp.broadcast_to(mass[:, b : b + 1], (maps, LANES))
    landed(acc_shared)
    for b in range(rows):
        total[b] = functools.reduce(
            jnp.add, [acc[s, b] * factor[s][:, b : b + 1] for s in range(n)]
        )

    averaged = []
    for i in range(maps):
        peak = peak_s[:, i, :]
        final = jnp.maximum(peak, own[i])
        keep = jnp.exp(peak - final)
        own_weight = jnp.exp(own[i] - final)
        at = (i // 2) * 2 * DH
        over = total[:, i, :] * keep + own_weight * new_values[:, at : at + 2 * DH]
        averaged.append(over / (sum_s[:, i, :] * keep + own_weight))
    heads = []
    gain = head_gain[...]
    for h in range(local_heads):
        difference = averaged[2 * h] - second_weight[:, h : h + 1] * averaged[2 * h + 1]
        inverse = lax.rsqrt(jnp.mean(difference * difference, axis=1, keepdims=True) + HEAD_EPSILON)
        heads.append((difference * inverse * gain * HEAD_SCALE).astype(BF16))
    attended = jnp.concatenate(heads, axis=1)

    out_copy.wait()
    att_x[side] = dot(attended, out_w[...]).astype(BF16)
    att_swap = swap(1, att_x.at[side], att_x.at[side])
    att_swap.wait_recv()
    mixed = (token_values + (att_x[0].astype(F32) + att_x[1].astype(F32))).astype(BF16)
    mixed_values = mixed.astype(F32)
    sq[me] = lane_total(mixed_values)
    sq_shared = share(4, sq)
    mixer_scaled = (mixed_values * mixer_gain).astype(BF16)

    gate_copy.wait()
    up_copy.wait()
    gu_shared = []
    for k, target in enumerate(peers + [me]):
        columns = pl.ds(pl.multiple_of(target * chunk, LANES), chunk)
        gate_part = dot(mixer_scaled, gate_w[:, columns])
        up_part = dot(mixer_scaled, up_w[:, columns])
        if k < n - 1:
            gu_out[k, :, :chunk] = gate_part.astype(BF16)
            gu_out[k, :, chunk:] = up_part.astype(BF16)
            gu_shared.append(push(5, k, gu_out.at[k], gu_in.at[k]))
    landed(sq_shared)
    mixer_total = functools.reduce(jnp.add, [sq[s] for s in range(n)])[:, :1]
    mixer_ratio = lax.rsqrt(mixer_total / model_width + NORM_EPSILON)
    for k in reversed(range(n - 1)):
        gu_shared[k].wait_recv()
        gate_part = gate_part + gu_in[k, :, :chunk].astype(F32)
        up_part = up_part + gu_in[k, :, chunk:].astype(F32)
    gate = gate_part * mixer_ratio
    hid[me] = (gate / (1.0 + jnp.exp(-gate)) * (up_part * mixer_ratio)).astype(BF16)
    hid_shared = share(6, hid)
    down_copy.wait()
    landed(hid_shared)
    term = None
    for s in range(n):
        depth = min(chunk, hidden_width - s * chunk)
        if depth > 0:
            piece = dot(hid[s][:, :depth], down_w[pl.ds(s * chunk, depth), :])
            term = piece if term is None else term + piece
    mix_x[side] = term.astype(BF16)
    mix_swap = swap(2, mix_x.at[side], mix_x.at[side])
    mix_swap.wait_recv()
    full = mixed_values + (mix_x[0].astype(F32) + mix_x[1].astype(F32))
    result[...] = jnp.where(side == 0, full[:, :width], full[:, width:])

    for copy in (
        [tok_swap, att_swap, mix_swap]
        + q_shared + kv_shared + acc_shared + stat_shared + sq_shared + gu_shared + hid_shared
    ):
        copy.wait_send()


def shards(
    n, tokens, attention_gain, query_one, query_two, key_one, key_two, value_weight,
    head_second_weight, head_gain, out_weight, mixer_gain, gate_weight, up_weight, down_weight,
    key_cache, value_cache,
):
    rows, width = tokens.shape
    positions, local_heads = key_cache.shape[1:3]
    maps = 2 * local_heads
    qw = query_one.shape[1]
    block = 2 * width
    hidden = gate_weight.shape[1]
    chunk = -(-hidden // (LANES * n)) * LANES
    table = jnp.asarray(rotary_table(positions * n, local_heads))
    span = positions * local_heads
    key_rows = key_cache.reshape(rows, span, 2 * DH)
    value_rows = value_cache.reshape(rows, span, 2 * DH)
    anywhere = pl.BlockSpec(memory_space=pl.ANY)
    inside = pl.BlockSpec(memory_space=pltpu.VMEM)
    vmem = pltpu.VMEM
    dma = pltpu.SemaphoreType.DMA
    weights = [query_one, query_two, key_one, key_two, value_weight, out_weight]
    return pl.pallas_call(
        functools.partial(layer, n),
        out_shape=jax.ShapeDtypeStruct((rows, width), F32),
        in_specs=[anywhere] * 17,
        out_specs=inside,
        scratch_shapes=[
            vmem(tokens.shape, BF16),
            vmem(attention_gain.shape, BF16),
            vmem(mixer_gain.shape, BF16),
            vmem(table.shape, F32),
            vmem((1, local_heads), F32),
            vmem((1, 2 * DH), F32),
            vmem((2, rows + 8, width), F32),
        ]
        + [vmem(w.shape, BF16) for w in weights]
        + [
            vmem((block, chunk * n), BF16),
            vmem((block, chunk * n), BF16),
            vmem(down_weight.shape, BF16),
            vmem((rows // 2, span, 2 * LANES), BF16),
            vmem((rows // 2, span, 2 * LANES), BF16),
            vmem((n, rows, 2 * qw + LANES), F32),
            vmem((n, rows, 2 * qw + value_weight.shape[1]), F32),
            vmem((rows, maps, LANES), F32),
            vmem((rows // 2, 2 * maps, span), F32),
            vmem((n, rows, maps, LANES), F32),
            vmem((n, maps, LANES), F32),
            vmem((rows, maps, LANES), F32),
            vmem((rows, maps, LANES), F32),
            vmem((rows, maps, LANES), F32),
            vmem((2, rows, block), BF16),
            vmem((n, rows, LANES), F32),
            vmem((n - 1, rows, 2 * chunk), BF16),
            vmem((n - 1, rows, 2 * chunk), BF16),
            vmem((n, rows, chunk), BF16),
            vmem((2, rows, block), BF16),
            dma((16,)),
            dma((rows,)),
            dma((rows,)),
            dma((3,)),
            dma((3,)),
            dma((7 + rows // 2, n - 1)),
            dma((7 + rows // 2, n - 1)),
        ],
        compiler_params=pltpu.CompilerParams(
            collective_id=0, has_side_effects=True, vmem_limit_bytes=60 * 1024 * 1024
        ),
    )(
        tokens, attention_gain, mixer_gain, table, head_second_weight[None], head_gain[None], query_one, query_two, key_one,
        key_two, value_weight, out_weight, gate_weight, up_weight, down_weight, key_rows, value_rows,
    ).astype(BF16)


def solution(mesh):
    placed = (
        P("dp", ("kv", "tp")),
        P(("kv", "tp")),
        P("kv", "tp"),
        P("kv", "tp"),
        P("kv", "tp"),
        P("kv", "tp"),
        P("kv", "tp"),
        P("tp"),
        P(),
        P("tp", "kv"),
        P(("kv", "tp")),
        P("kv", "tp"),
        P("kv", "tp"),
        P("tp", "kv"),
        P("dp", "kv", "tp", None),
        P("dp", "kv", "tp", None),
    )
    return jax.shard_map(
        functools.partial(shards, mesh.shape["kv"]),
        mesh=mesh, in_specs=placed, out_specs=P("dp", ("kv", "tp")), check_vma=False,
    )
```

```python
import functools

import jax
import jax.numpy as jnp
import numpy as np
from jax import lax
from jax.experimental import pallas as pl
from jax.experimental.pallas import tpu as pltpu
from jax.sharding import PartitionSpec as P

DH = 64
LANES = 128

NORM_EPSILON = 1e-06
HEAD_EPSILON = 1e-05
HEAD_SCALE = 0.8
ROTARY_BASE = 10000.0

F32 = jnp.float32
BF16 = jnp.bfloat16


def rotary_table(position, local_heads):
    half = DH // 2
    frequency = np.float32(1.0) / np.float32(ROTARY_BASE) ** (np.arange(half, dtype=np.float32) / np.float32(half))
    angles = (np.float32(position) * frequency).astype(np.float32).astype(np.float64)
    cosine = np.concatenate([np.cos(angles), np.cos(angles)])
    sine = np.concatenate([-np.sin(angles), np.sin(angles)])
    return np.stack([np.tile(cosine, local_heads), np.tile(sine, local_heads)]).astype(np.float32)


def peer_order(me, n):
    assert n & (n - 1) == 0
    order = []
    for flip in range(n - 1, 0, -1):
        target = me
        bit = 1
        while bit < n:
            if flip & bit:
                target = target + bit - 2 * bit * lax.rem(me // bit, 2)
            bit *= 2
        order.append(target)
    return order


def dot(left, right):
    return jnp.dot(left, right, preferred_element_type=F32)


def layer(
    n, tokens_h, first_gain_h, second_gain_h, table_h, second_weight_h, head_gain_h, q1_h, q2_h, k1_h, k2_h, v_h, out_h, gate_h, up_h,
    down_h, key_h, value_h, result,
    raw_tokens, raw_first, raw_second, table, second_weight, head_gain, tok, q1_w, q2_w, k1_w, k2_w, v_w, out_w, gate_w, up_w, down_w, keys, values,
    q_part, kv_part, v_part, q_pad, scores, acc, stats, total, peak_s, sum_s, att_x, sq, gu_out, gu_in,
    hid, mix_x, load, key_sem, value_sem, tp_send, tp_recv, kv_send, kv_recv,
):
    rows, width = tokens_h.shape
    local_heads = q1_h.shape[1] // DH
    maps = 2 * local_heads
    me = lax.axis_index("kv")
    side = lax.axis_index("tp")
    other = 1 - side
    model_width = width * 2 * n
    hidden_width = gate_h.shape[1]
    chunk = hid.shape[2]

    peers = peer_order(me, n)
    barrier = pltpu.get_barrier_semaphore()
    for target in peers:
        pl.semaphore_signal(barrier, inc=1, device_id={"kv": target})
    pl.semaphore_signal(barrier, inc=1, device_id={"tp": other})

    def fetch(source, target, sem):
        copy = pltpu.make_async_copy(source, target, sem)
        copy.start()
        return copy

    small = [
        fetch(source, target, load.at[10 + i])
        for i, (source, target) in enumerate(
            (
                (tokens_h, raw_tokens), (first_gain_h, raw_first), (second_gain_h, raw_second),
                (table_h, table), (second_weight_h, second_weight), (head_gain_h, head_gain),
            )
        )
    ]
    loads = [
        fetch(source, target, load.at[i])
        for i, (source, target) in enumerate(
            ((q1_h, q1_w), (q2_h, q2_w), (k1_h, k1_w), (k2_h, k2_w), (v_h, v_w))
        )
    ]
    for copy in small:
        copy.wait()
    tok[side, :rows] = raw_tokens[...].astype(F32)
    tok[side, rows : rows + 1] = raw_first[...].astype(F32).reshape(1, width)
    tok[side, rows + 1 : rows + 2] = raw_second[...].astype(F32).reshape(1, width)
    tok[side, rows + 2 :] = jnp.zeros((6, width), F32)
    pl.semaphore_wait(barrier, n)

    def swap(phase, source, target):
        copy = pltpu.make_async_remote_copy(
            src_ref=source, dst_ref=target, send_sem=tp_send.at[phase],
            recv_sem=tp_recv.at[phase], device_id={"tp": other},
        )
        copy.start()
        return copy

    def push(phase, k, source, target):
        copy = pltpu.make_async_remote_copy(
            src_ref=source, dst_ref=target, send_sem=kv_send.at[phase, k],
            recv_sem=kv_recv.at[phase, k], device_id={"kv": peers[k]},
        )
        copy.start()
        return copy

    def share(phase, buffer):
        return [push(phase, k, buffer.at[me], buffer.at[me]) for k in range(n - 1)]

    def landed(copies):
        for copy in copies:
            copy.wait_recv()

    sent = []
    tok_swap = swap(0, tok.at[side], tok.at[side])
    key_copies = [
        fetch(key_h.at[b], keys.at[b // 2, :, pl.ds(b % 2 * LANES, LANES)], key_sem.at[b])
        for b in range(rows)
    ]
    value_copies = [
        fetch(value_h.at[b], values.at[b // 2, :, pl.ds(b % 2 * LANES, LANES)], value_sem.at[b])
        for b in range(rows)
    ]
    out_copy = fetch(out_h, out_w, load.at[6])
    gate_copy = fetch(gate_h, gate_w.at[:, pl.ds(0, hidden_width)], load.at[7])
    up_copy = fetch(up_h, up_w.at[:, pl.ds(0, hidden_width)], load.at[8])
    down_copy = fetch(down_h, down_w, load.at[9])
    if chunk * n > hidden_width:
        pad = chunk * n - hidden_width
        gate_w[:, hidden_width:] = jnp.zeros((gate_w.shape[0], pad), BF16)
        up_w[:, hidden_width:] = jnp.zeros((up_w.shape[0], pad), BF16)
    tok_swap.wait_recv()
    block = jnp.concatenate([tok[0], tok[1]], axis=1)
    token_values = block[:rows]
    scaled = (token_values * block[rows : rows + 1]).astype(BF16)
    mixer_gain = block[rows + 1 : rows + 2]

    def lane_total(x):
        return jnp.broadcast_to(jnp.sum(x * x, axis=1, keepdims=True), (rows, LANES))

    qw = q1_h.shape[1]
    vw = v_h.shape[1]
    loads[0].wait()
    q_part[me, :, :qw] = dot(scaled, q1_w[...])
    loads[1].wait()
    q_part[me, :, qw : 2 * qw] = dot(scaled, q2_w[...])
    q_part[me, :, 2 * qw :] = lane_total(token_values)
    q_shared = share(0, q_part)
    loads[2].wait()
    kv_part[me, :, :qw] = dot(scaled, k1_w[...])
    loads[3].wait()
    kv_part[me, :, qw : 2 * qw] = dot(scaled, k2_w[...])
    kv_shared = share(1, kv_part)
    loads[4].wait()
    v_part[me] = dot(scaled, v_w[...]).astype(BF16)
    kv_shared += share(2, v_part)

    cosine = table[0:1, :]
    sine = table[1:2, :]
    lane = lax.broadcasted_iota(jnp.int32, (rows, qw), 1)
    lead = lax.rem(lane, DH) < DH // 2
    tile_lane = lax.broadcasted_iota(jnp.int32, (rows, LANES), 1)
    low = tile_lane < DH

    def rotated(x):
        turned = jnp.where(lead, pltpu.roll(x, qw - DH // 2, 1), pltpu.roll(x, DH // 2, 1))
        return (x * cosine + turned * sine).astype(BF16).astype(F32)

    def padded(first, second):
        tiles = []
        for h in range(local_heads):
            at = (h // 2) * LANES
            one = first[:, at : at + LANES]
            two = second[:, at : at + LANES]
            if h % 2:
                one = pltpu.roll(one, DH, 1)
            else:
                two = pltpu.roll(two, DH, 1)
            tiles.append(jnp.where(low, one, 0.0))
            tiles.append(jnp.where(low, 0.0, two))
        return tiles

    landed(q_shared)
    q_sum = functools.reduce(jnp.add, [q_part[s] for s in range(n)])
    ratio = lax.rsqrt(q_sum[:, 2 * qw : 2 * qw + 1] / model_width + NORM_EPSILON)
    queries = padded(rotated(q_sum[:, :qw] * ratio), rotated(q_sum[:, qw : 2 * qw] * ratio))
    for i in range(maps):
        q_pad[:, i, :] = queries[i]

    span = keys.shape[1]
    score_scale = DH ** (-0.5)
    pair = 2 * maps
    row_head = lax.rem(lax.broadcasted_iota(jnp.int32, (pair, span), 0), maps) // 2
    col_head = lax.rem(lax.broadcasted_iota(jnp.int32, (pair, span), 1), local_heads)
    mine = row_head == col_head
    stat_lane = lax.broadcasted_iota(jnp.int32, (maps, LANES), 1)
    stat = jnp.zeros((maps, LANES), F32)
    blank = jnp.zeros((maps, LANES), F32)
    acc_shared = []

    def score(g):
        key_copies[2 * g].wait()
        key_copies[2 * g + 1].wait()
        query = jnp.concatenate(
            [
                jnp.concatenate([q_pad[2 * g], blank], axis=1),
                jnp.concatenate([blank, q_pad[2 * g + 1]], axis=1),
            ],
            axis=0,
        ).astype(BF16)
        raw = lax.dot_general(
            query, keys[g], (((1,), (1,)), ((), ())), preferred_element_type=F32
        )
        scores[g] = jnp.where(mine, raw * score_scale, -jnp.inf)

    groups = rows // 2
    score(0)
    for g in range(groups):
        if g + 1 < groups:
            score(g + 1)
        value_copies[2 * g].wait()
        value_copies[2 * g + 1].wait()
        logit = scores[g]
        peak = jnp.max(logit, axis=1, keepdims=True)
        weight = jnp.exp(logit - peak)
        weight_sum = jnp.sum(weight, axis=1, keepdims=True)
        both = dot(weight.astype(BF16), values[g])
        for j in range(2):
            part = slice(j * maps, (j + 1) * maps)
            acc[me, 2 * g + j] = both[part, j * LANES : (j + 1) * LANES]
            stat = jnp.where(stat_lane == 2 * g + j, peak[part], stat)
            stat = jnp.where(stat_lane == rows + 2 * g + j, weight_sum[part], stat)
        if g + 1 == groups:
            stats[me] = stat
            stat_shared = share(3, stats)
        pieces = acc.at[me, pl.ds(2 * g, 2)]
        acc_shared += [push(7 + g, k, pieces, pieces) for k in range(n - 1)]

    landed(kv_shared)
    kv_sum = functools.reduce(jnp.add, [kv_part[s] for s in range(n)])
    new_keys = padded(rotated(kv_sum[:, :qw] * ratio), rotated(kv_sum[:, qw : 2 * qw] * ratio))
    v_sum = functools.reduce(jnp.add, [v_part[s].astype(F32) for s in range(n)])
    new_values = (v_sum * ratio).astype(BF16).astype(F32)
    own = [
        jnp.sum(queries[i] * new_keys[i], axis=1, keepdims=True) * score_scale for i in range(maps)
    ]

    landed(stat_shared)
    every = [stats[s] for s in range(n)]
    top = functools.reduce(jnp.maximum, every)
    is_peak = stat_lane < rows
    factor = [jnp.exp(jnp.where(is_peak, every[s] - top, 0.0)) for s in range(n)]
    sums = [pltpu.roll(every[s], LANES - rows, 1) for s in range(n)]
    mass = functools.reduce(jnp.add, [factor[s] * sums[s] for s in range(n)])
    for b in range(rows):
        peak_s[b] = jnp.broadcast_to(top[:, b : b + 1], (maps, LANES))
        sum_s[b] = jnp.broadcast_to(mass[:, b : b + 1], (maps, LANES))
    landed(acc_shared)
    for b in range(rows):
        total[b] = functools.reduce(
            jnp.add, [acc[s, b] * factor[s][:, b : b + 1] for s in range(n)]
        )

    averaged = []
    for i in range(maps):
        peak = peak_s[:, i, :]
        final = jnp.maximum(peak, own[i])
        keep = jnp.exp(peak - final)
        own_weight = jnp.exp(own[i] - final)
        at = (i // 2) * 2 * DH
        over = total[:, i, :] * keep + own_weight * new_values[:, at : at + 2 * DH]
        averaged.append(over / (sum_s[:, i, :] * keep + own_weight))
    heads = []
    gain = head_gain[...]
    for h in range(local_heads):
        difference = averaged[2 * h] - second_weight[:, h : h + 1] * averaged[2 * h + 1]
        inverse = lax.rsqrt(jnp.mean(difference * difference, axis=1, keepdims=True) + HEAD_EPSILON)
        heads.append((difference * inverse * gain * HEAD_SCALE).astype(BF16))
    attended = jnp.concatenate(heads, axis=1)

    out_copy.wait()
    att_x[side] = dot(attended, out_w[...]).astype(BF16)
    att_swap = swap(1, att_x.at[side], att_x.at[side])
    att_swap.wait_recv()
    mixed = (token_values + (att_x[0].astype(F32) + att_x[1].astype(F32))).astype(BF16)
    mixed_values = mixed.astype(F32)
    sq[me] = lane_total(mixed_values)
    sq_shared = share(4, sq)
    mixer_scaled = (mixed_values * mixer_gain).astype(BF16)

    gate_copy.wait()
    up_copy.wait()
    gu_shared = []
    for k, target in enumerate(peers + [me]):
        columns = pl.ds(pl.multiple_of(target * chunk, LANES), chunk)
        gate_part = dot(mixer_scaled, gate_w[:, columns])
        up_part = dot(mixer_scaled, up_w[:, columns])
        if k < n - 1:
            gu_out[k, :, :chunk] = gate_part.astype(BF16)
            gu_out[k, :, chunk:] = up_part.astype(BF16)
            gu_shared.append(push(5, k, gu_out.at[k], gu_in.at[k]))
    landed(sq_shared)
    mixer_total = functools.reduce(jnp.add, [sq[s] for s in range(n)])[:, :1]
    mixer_ratio = lax.rsqrt(mixer_total / model_width + NORM_EPSILON)
    for k in reversed(range(n - 1)):
        gu_shared[k].wait_recv()
        gate_part = gate_part + gu_in[k, :, :chunk].astype(F32)
        up_part = up_part + gu_in[k, :, chunk:].astype(F32)
    gate = gate_part * mixer_ratio
    hid[me] = (gate / (1.0 + jnp.exp(-gate)) * (up_part * mixer_ratio)).astype(BF16)
    hid_shared = share(6, hid)
    down_copy.wait()
    landed(hid_shared)
    term = None
    for s in range(n):
        depth = min(chunk, hidden_width - s * chunk)
        if depth > 0:
            piece = dot(hid[s][:, :depth], down_w[pl.ds(s * chunk, depth), :])
            term = piece if term is None else term + piece
    mix_x[side] = term.astype(BF16)
    mix_swap = swap(2, mix_x.at[side], mix_x.at[side])
    mix_swap.wait_recv()
    full = mixed_values + (mix_x[0].astype(F32) + mix_x[1].astype(F32))
    result[...] = jnp.where(side == 0, full[:, :width], full[:, width:])

    for copy in (
        [tok_swap, att_swap, mix_swap]
        + q_shared + kv_shared + acc_shared + stat_shared + sq_shared + gu_shared + hid_shared
    ):
        copy.wait_send()


def shards(
    n, tokens, attention_gain, query_one, query_two, key_one, key_two, value_weight,
    head_second_weight, head_gain, out_weight, mixer_gain, gate_weight, up_weight, down_weight,
    key_cache, value_cache,
):
    rows, width = tokens.shape
    positions, local_heads = key_cache.shape[1:3]
    maps = 2 * local_heads
    qw = query_one.shape[1]
    block = 2 * width
    hidden = gate_weight.shape[1]
    chunk = -(-hidden // (LANES * n)) * LANES
    table = jnp.asarray(rotary_table(positions * n, local_heads))
    span = positions * local_heads
    key_rows = key_cache.reshape(rows, span, 2 * DH)
    value_rows = value_cache.reshape(rows, span, 2 * DH)
    anywhere = pl.BlockSpec(memory_space=pl.ANY)
    inside = pl.BlockSpec(memory_space=pltpu.VMEM)
    vmem = pltpu.VMEM
    dma = pltpu.SemaphoreType.DMA
    weights = [query_one, query_two, key_one, key_two, value_weight, out_weight]
    return pl.pallas_call(
        functools.partial(layer, n),
        out_shape=jax.ShapeDtypeStruct((rows, width), F32),
        in_specs=[anywhere] * 17,
        out_specs=inside,
        scratch_shapes=[
            vmem(tokens.shape, BF16),
            vmem(attention_gain.shape, BF16),
            vmem(mixer_gain.shape, BF16),
            vmem(table.shape, F32),
            vmem((1, local_heads), F32),
            vmem((1, 2 * DH), F32),
            vmem((2, rows + 8, width), F32),
        ]
        + [vmem(w.shape, BF16) for w in weights]
        + [
            vmem((block, chunk * n), BF16),
            vmem((block, chunk * n), BF16),
            vmem(down_weight.shape, BF16),
            vmem((rows // 2, span, 2 * LANES), BF16),
            vmem((rows // 2, span, 2 * LANES), BF16),
            vmem((n, rows, 2 * qw + LANES), F32),
            vmem((n, rows, 2 * qw), F32),
            vmem((n, rows, value_weight.shape[1]), BF16),
            vmem((rows, maps, LANES), F32),
            vmem((rows // 2, 2 * maps, span), F32),
            vmem((n, rows, maps, LANES), F32),
            vmem((n, maps, LANES), F32),
            vmem((rows, maps, LANES), F32),
            vmem((rows, maps, LANES), F32),
            vmem((rows, maps, LANES), F32),
            vmem((2, rows, block), BF16),
            vmem((n, rows, LANES), F32),
            vmem((n - 1, rows, 2 * chunk), BF16),
            vmem((n - 1, rows, 2 * chunk), BF16),
            vmem((n, rows, chunk), BF16),
            vmem((2, rows, block), BF16),
            dma((16,)),
            dma((rows,)),
            dma((rows,)),
            dma((3,)),
            dma((3,)),
            dma((7 + rows // 2, n - 1)),
            dma((7 + rows // 2, n - 1)),
        ],
        compiler_params=pltpu.CompilerParams(
            collective_id=0, has_side_effects=True, vmem_limit_bytes=60 * 1024 * 1024
        ),
    )(
        tokens, attention_gain, mixer_gain, table, head_second_weight[None], head_gain[None], query_one, query_two, key_one,
        key_two, value_weight, out_weight, gate_weight, up_weight, down_weight, key_rows, value_rows,
    ).astype(BF16)


def solution(mesh):
    placed = (
        P("dp", ("kv", "tp")),
        P(("kv", "tp")),
        P("kv", "tp"),
        P("kv", "tp"),
        P("kv", "tp"),
        P("kv", "tp"),
        P("kv", "tp"),
        P("tp"),
        P(),
        P("tp", "kv"),
        P(("kv", "tp")),
        P("kv", "tp"),
        P("kv", "tp"),
        P("tp", "kv"),
        P("dp", "kv", "tp", None),
        P("dp", "kv", "tp", None),
    )
    return jax.shard_map(
        functools.partial(shards, mesh.shape["kv"]),
        mesh=mesh, in_specs=placed, out_specs=P("dp", ("kv", "tp")), check_vma=False,
    )
```
